32 devices in a mesh: sp: 4 (over z), tp: 8 (over y, x, core).
Axes of the slice: x: 2, y: 2, z: 4, core: 2. Of those that a mesh axis runs over, the one named last changes fastest.
Arguments:
- tokens: bfloat16 [3072, 2048], P('sp'), may hold values from -6 to 6
- norm_gain: float32 [2048], replicated, may hold values from 0.5 to 80
- grid_query_weight: bfloat16 [2048, 2048], P(None, 'tp'), may hold values from -0.5 to 0.5
- grid_key_weight: bfloat16 [2048, 1024], P(None, 'tp'), may hold values from -0.5 to 0.5
- grid_value_weight: bfloat16 [2048, 1024], P(None, 'tp'), may hold values from -0.5 to 0.5
- grid_query_gain: float32 [128], replicated, may hold values from 1.6 to 6
- grid_key_gain: float32 [128], replicated, may hold values from 1.6 to 6
- local_query_weight: bfloat16 [2048, 2048], P(None, 'tp'), may hold values from -0.5 to 0.5
- local_key_weight: bfloat16 [2048, 1024], P(None, 'tp'), may hold values from -0.5 to 0.5
- local_value_weight: bfloat16 [2048, 1024], P(None, 'tp'), may hold values from -0.5 to 0.5
- sink_logit: float32 [16], P('tp'), may hold values from 1 to 6
- grid_out_weight: bfloat16 [2048, 2048], P('tp'), may hold values from -0.09375 to 0.09375
- local_out_weight: bfloat16 [2048, 2048], P('tp'), may hold values from -0.09375 to 0.09375
Outputs:
- mixed: bfloat16 [3072, 2048], P(('sp', 'tp'))
The draws below stay inside these ranges and needn't reach their ends.
All inputs are finite; a program needn't handle non-finite values.
Results may differ from the reference program's by a relative error of at most 0.03.
Values may be sent and summed in bfloat16 or wider, within the bound.
A program may use at most 192 MiB of HBM per device.

```python
import jax
import jax.numpy as jnp
from jax import lax

D = 2048
HEAD = 128
GRID_HEADS = 16
GRID_KV = 8
LOCAL_HEADS = 16
LOCAL_KV = 8
WINDOW = 128
GRID_W = 64
SEQ = 3072
N_TP = 8


def shared_weight(key, salt, heads):
    drawn = jax.random.normal(jax.random.fold_in(key, salt), (D, heads * HEAD), jnp.float32) * D ** (-0.5)
    return jnp.clip(drawn, -0.5, 0.5)


def paired_key(key, salt, heads, groups):
    return shared_weight(key, salt + 1, groups)


def draw_grid_query_weight(key, part):
    return shared_weight(key, 101, GRID_HEADS).astype(jnp.bfloat16)


def draw_grid_key_weight(key, part):
    return paired_key(key, 101, GRID_HEADS, GRID_KV).astype(jnp.bfloat16)


def draw_local_query_weight(key, part):
    return shared_weight(key, 301, LOCAL_HEADS).astype(jnp.bfloat16)


def draw_local_key_weight(key, part):
    return paired_key(key, 301, LOCAL_HEADS, LOCAL_KV).astype(jnp.bfloat16)


def draw_norm_gain(key, part):
    base = jax.random.uniform(jax.random.fold_in(key, 201), (D,), jnp.float32, 0.5, 1.5)
    return base


def head_gain(key, salt):
    return jax.random.uniform(jax.random.fold_in(key, salt), (HEAD,), jnp.float32, 1.6, 2.4)


def draw_grid_query_gain(key, part):
    return head_gain(key, 401)


def draw_grid_key_gain(key, part):
    return head_gain(key, 402)


def level_of(key, dims, pieces, low, high):
    def one(dim, parts):
        draws = jax.random.uniform(jax.random.fold_in(jax.random.fold_in(key, 6), dim), (parts,), jnp.float32, low / len(pieces), high / len(pieces))
        return jnp.repeat(jnp.exp(draws), dims[dim] // parts).reshape((-1,) + (1,) * (len(dims) - dim - 1))

    level = one(*pieces[0])
    for cut in pieces[1:]:
        level = level * one(*cut)
    return level


def normal_values(key, dims, scale, reach, cuts=(), kind=jnp.bfloat16):
    entries = scale * jax.random.normal(key, dims, jnp.float32)
    if cuts:
        entries = entries * level_of(key, dims, cuts, -0.22, 0.18)
    return jnp.clip(entries, -reach, reach).astype(kind)


def setup_inputs(seed: int = 0) -> dict:
    key_list = jax.random.split(jax.random.key(seed), 14)
    return {
        "tokens": normal_values(key_list[0], (SEQ, D), 1.0, 6.0, ((0, 4),)),
        "norm_gain": draw_norm_gain(jax.random.fold_in(key_list[13], 71), 0),
        "grid_query_weight": draw_grid_query_weight(jax.random.fold_in(key_list[13], 71), 0),
        "grid_key_weight": draw_grid_key_weight(jax.random.fold_in(key_list[13], 71), 0),
        "grid_value_weight": normal_values(key_list[4], (D, GRID_KV * HEAD), (D // 16) ** -0.5, 0.5, ((1, 8),)),
        "grid_query_gain": draw_grid_query_gain(jax.random.fold_in(key_list[13], 71), 0),
        "grid_key_gain": draw_grid_key_gain(jax.random.fold_in(key_list[13], 71), 0),
        "local_query_weight": draw_local_query_weight(jax.random.fold_in(key_list[13], 71), 0),
        "local_key_weight": draw_local_key_weight(jax.random.fold_in(key_list[13], 71), 0),
        "local_value_weight": normal_values(key_list[9], (D, LOCAL_KV * HEAD), (D // 16) ** -0.5, 0.5, ((1, 8),)),
        "sink_logit": jnp.clip(1.0 + 5.0 * jax.random.uniform(key_list[10], (LOCAL_HEADS,), jnp.float32) ** level_of(key_list[10], (LOCAL_HEADS,), ((0, 8),), -0.2, 0.2), 1.0, 6.0),
        "grid_out_weight": normal_values(key_list[11], (GRID_HEADS * HEAD, D), (GRID_HEADS * HEAD + LOCAL_HEADS * HEAD) ** -0.5, 0.09375, ((0, 8),)),
        "local_out_weight": normal_values(key_list[12], (LOCAL_HEADS * HEAD, D), (GRID_HEADS * HEAD + LOCAL_HEADS * HEAD) ** -0.5, 0.09375, ((0, 8),)),
    }


EPSILON = 1e-06
ROPE_BASE = 10000.0

def rms_rows(values, gain):
    widened = values.astype(jnp.float32)
    return widened * lax.rsqrt(lax.optimization_barrier(jnp.mean(widened * widened, axis=-1, keepdims=True)) + EPSILON) * gain

def half_turn(part, angles):
    cosine = jnp.cos(angles)
    sine = jnp.sin(angles)
    cosine = jnp.concatenate([cosine, cosine], axis=-1)
    sine = jnp.concatenate([sine, sine], axis=-1)
    first, second = jnp.split(part, 2, axis=-1)
    turned = jnp.concatenate([-second, first], axis=-1)
    return part * cosine + turned * sine

def axial_turn(heads, positions):
    half_dim = heads.shape[-1] // 2
    inverse = ROPE_BASE ** (-jnp.arange(0, half_dim, 2, dtype=jnp.float32) / half_dim)
    row_angle = (positions // GRID_W).astype(jnp.float32)[:, None, None] * inverse
    col_angle = (positions % GRID_W).astype(jnp.float32)[:, None, None] * inverse
    return jnp.concatenate([half_turn(heads[..., :half_dim], row_angle), half_turn(heads[..., half_dim:], col_angle)], axis=-1)

def rounded_part(outs, weight, index, width):
    picked = lax.dynamic_slice_in_dim(outs, (index * width).astype(jnp.int32), width, 1)
    rows = lax.dynamic_slice_in_dim(weight, (index * width).astype(jnp.int32), width, 0)
    product = jnp.dot(picked, rows, preferred_element_type=jnp.float32).astype(jnp.bfloat16)
    return lax.optimization_barrier(product).astype(jnp.float32)

def reference(tokens, norm_gain, grid_query_weight, grid_key_weight, grid_value_weight, grid_query_gain, grid_key_gain, local_query_weight, local_key_weight, local_value_weight, sink_logit, grid_out_weight, local_out_weight):
    seq_len = tokens.shape[0]
    positions = jnp.arange(seq_len, dtype=jnp.int32)
    normed = rms_rows(tokens, norm_gain).astype(jnp.bfloat16)

    def project(weight):
        return jnp.dot(normed, weight, preferred_element_type=jnp.float32).astype(jnp.bfloat16)
    group_size = GRID_HEADS // GRID_KV
    score_scale = HEAD ** (-0.5)
    queries = axial_turn(rms_rows(project(grid_query_weight).reshape(seq_len, GRID_HEADS, HEAD), grid_query_gain), positions).astype(jnp.bfloat16).reshape(seq_len, GRID_KV, group_size, HEAD)
    keys = axial_turn(rms_rows(project(grid_key_weight).reshape(seq_len, GRID_KV, HEAD), grid_key_gain), positions).astype(jnp.bfloat16)
    values = project(grid_value_weight).reshape(seq_len, GRID_KV, HEAD)
    keys_wide = keys.astype(jnp.float32)
    values_wide = values.astype(jnp.float32)
    block_rows = min(512, seq_len)

    def one_block(start):
        block_q = lax.dynamic_slice_in_dim(queries, start, block_rows, 0).astype(jnp.float32)
        scores = jnp.einsum('qhgd,shd->hgqs', block_q, keys_wide) * score_scale
        weights = jax.nn.softmax(scores, axis=-1).astype(jnp.bfloat16)
        result = jnp.einsum('hgqs,shd->qhgd', weights.astype(jnp.float32), values_wide)
        return result.astype(jnp.bfloat16)
    starts = (jnp.arange(seq_len // block_rows) * block_rows).astype(jnp.int32)
    grid_out = lax.map(one_block, starts).reshape(seq_len, GRID_HEADS * HEAD)
    local_size = LOCAL_HEADS // LOCAL_KV
    blocks = seq_len // WINDOW
    local_q = project(local_query_weight).reshape(blocks, WINDOW, LOCAL_KV, local_size, HEAD)
    local_k = project(local_key_weight).reshape(seq_len, LOCAL_KV, HEAD)
    local_v = project(local_value_weight).reshape(seq_len, LOCAL_KV, HEAD)

    def banded(values_in):
        padded = jnp.pad(values_in, ((WINDOW, WINDOW), (0, 0), (0, 0))).reshape(blocks + 2, WINDOW, LOCAL_KV, HEAD)
        return jnp.concatenate([padded[:-2], padded[1:-1], padded[2:]], axis=1)
    band_k = banded(local_k).astype(jnp.float32)
    band_v = banded(local_v).astype(jnp.float32)
    scores = jnp.einsum('nqhgd,nshd->hgnqs', local_q.astype(jnp.float32), band_k) * score_scale
    relative = jnp.arange(3 * WINDOW)[None, :] - WINDOW - jnp.arange(WINDOW)[:, None]
    key_pos = jnp.arange(blocks)[:, None] * WINDOW - WINDOW + jnp.arange(3 * WINDOW)[None, :]
    valid = (jnp.abs(relative) <= WINDOW)[None] & ((key_pos >= 0) & (key_pos < seq_len))[:, None, :]
    scores = jnp.where(valid, scores, -jnp.inf)
    sink = sink_logit.reshape(LOCAL_KV, local_size, 1, 1, 1)
    top = jnp.maximum(lax.optimization_barrier(jnp.max(scores, axis=-1, keepdims=True)), sink)
    lifted = jnp.exp(scores - top)
    weights = (lifted / (lax.optimization_barrier(jnp.sum(lifted, axis=-1, keepdims=True)) + jnp.exp(sink - top))).astype(jnp.bfloat16)
    local_out = jnp.einsum('hgnqs,nshd->nqhgd', weights.astype(jnp.float32), band_v)
    local_out = local_out.astype(jnp.bfloat16).reshape(seq_len, LOCAL_HEADS * HEAD)
    grid_width = GRID_HEADS * HEAD // N_TP
    local_width = LOCAL_HEADS * HEAD // N_TP

    def add_group(index, total):
        total = total + rounded_part(grid_out, grid_out_weight, index, grid_width)
        return total + rounded_part(local_out, local_out_weight, index, local_width)
    total = lax.fori_loop(0, N_TP, add_group, jnp.zeros((seq_len, D), jnp.float32))
    return total.astype(jnp.bfloat16)
```

```python
import functools

import jax
import jax.numpy as jnp
import numpy as np
from jax import lax
from jax.experimental import pallas as pl
from jax.experimental.pallas import tpu as pltpu
from jax.sharding import PartitionSpec as P

HEAD = 128
WINDOW = 128
GRID_W = 64
EPSILON = 1e-06
ROPE_BASE = 10000.0
PIECE = 32
CHUNK = 256
LOG2E = 1.4426950408889634
SCALE = HEAD ** (-0.5)
MESH = pl.DeviceIdType.MESH


def rotary_tables(total_rows):
    half = HEAD // 2
    inverse = (ROPE_BASE ** (-np.arange(0, half, 2, dtype=np.float32) / half)).astype(np.float32)

    def table(count, low):
        angle = np.arange(count, dtype=np.float32)[:, None] * inverse
        cosine = np.cos(angle).astype(np.float32)
        sine = np.sin(angle).astype(np.float32)
        zero = np.zeros((count, half), np.float32)
        cosine = np.concatenate([cosine, cosine], axis=1)
        sine = np.concatenate([-sine, sine], axis=1)
        order = (lambda x: [x, zero]) if low else (lambda x: [zero, x])
        return np.stack(
            [np.concatenate(order(cosine), axis=1), np.concatenate(order(sine), axis=1)]
        )

    return table(total_rows // GRID_W, True), table(GRID_W, False)


def dot(a, b):
    return jnp.dot(a, b, preferred_element_type=jnp.float32)


def dot_t(a, b):
    return lax.dot_general(a, b, (((1,), (1,)), ((), ())), preferred_element_type=jnp.float32)


def with_ones(v):
    return jnp.concatenate([v, jnp.ones((v.shape[0], HEAD), v.dtype)], axis=1)


def kernel(
    n_sp, n_tp, rows, width,
    tokens, gain, gqw, gkw, gvw, gq_gain, gk_gain, lqw, lkw, lvw, sink, gow, low, row_tab, col_tab,
    out,
    tok_v, normed, wkv, wq, wo, kv, lkv, q_s, lq_s, lo_s, acc, m_s, pbuf, rbuf0, sbuf, rbuf1,
    in_sem, kv_recv, kv_send, fwd_send, halo_recv, halo_send, r0_send, r0_recv, r1_send, r1_recv,
):
    me = lax.axis_index("sp")
    tp = lax.axis_index("tp")
    par = lax.rem(tp, 2)
    chip = tp // 2
    chips = n_tp // 2
    units = rows // (n_tp * PIECE)
    unit_rows = n_tp * PIECE
    partner = tp + 1 - 2 * par

    chunks = rows // CHUNK
    loads = []

    def load(src, dst):
        copy = pltpu.make_async_copy(src, dst, in_sem.at[len(loads)])
        copy.start()
        loads.append(copy)

    load(tokens.at[pl.ds(0, CHUNK)], tok_v.at[pl.ds(0, CHUNK)])
    for i, w in enumerate((gkw, gvw, lkw, lvw)):
        load(w, wkv.at[:, pl.ds(i * HEAD, HEAD)])
    load(tokens.at[pl.ds(CHUNK, rows - CHUNK)], tok_v.at[pl.ds(CHUNK, rows - CHUNK)])
    load(gqw, wq.at[:, pl.ds(0, 2 * HEAD)])
    load(lqw, wq.at[:, pl.ds(2 * HEAD, 2 * HEAD)])
    load(gow, wo.at[pl.ds(0, 2 * HEAD)])
    load(low, wo.at[pl.ds(2 * HEAD, 2 * HEAD)])

    barrier = pltpu.get_barrier_semaphore()
    for step in (-2, -1, 1, 2):
        other = me + step

        @pl.when((other >= 0) & (other < n_sp))
        def _():
            pl.semaphore_signal(barrier, inc=1, device_id={"sp": other}, device_id_type=MESH)

    pl.semaphore_signal(barrier, inc=1, device_id={"tp": partner}, device_id_type=MESH)
    for k in range(1, chips):
        peer = lax.rem(chip + k, chips) * 2 + par
        pl.semaphore_signal(barrier, inc=1, device_id={"tp": peer}, device_id_type=MESH)
    near = jnp.minimum(me, 2) + jnp.minimum(n_sp - 1 - me, 2)
    pl.semaphore_wait(barrier, near + chips)

    def norm_heads(x, head_gain):
        return x * lax.rsqrt(jnp.mean(x * x, axis=-1, keepdims=True) + EPSILON) * head_gain

    def rotary(x, group, count):
        def tiled(k):
            return jnp.concatenate(
                [row_tab[k, pl.ds(group + i, 1), :] + col_tab[k] for i in range(count // GRID_W)],
                axis=0,
            )

        lane = lax.broadcasted_iota(jnp.int32, x.shape, 1)
        quarter = HEAD // 4
        first = lax.rem(lane, 2 * quarter) < quarter
        turned = jnp.where(
            first, pltpu.roll(x, HEAD - quarter, 1), pltpu.roll(x, quarter, 1)
        )
        return x * tiled(0) + turned * tiled(1)

    def place(g):
        t = g // units
        return lax.rem(g, units), lax.rem(t, 2) * chips + t // 2

    first_group = me * (rows // GRID_W)

    loads[0].wait()
    for i in range(1, 5):
        loads[i].wait()

    def kv_chunk(c):
        at = pl.multiple_of(c * CHUNK, CHUNK)
        wide = tok_v[pl.ds(at, CHUNK), :].astype(jnp.float32)
        mean = jnp.mean(wide * wide, axis=-1, keepdims=True)
        scaled = (wide * lax.rsqrt(mean + EPSILON) * gain[...]).astype(jnp.bfloat16)
        normed[pl.ds(at, CHUNK), :] = scaled
        made = dot(scaled, wkv[...]).astype(jnp.bfloat16)
        key = norm_heads(made[:, :HEAD].astype(jnp.float32), gk_gain[...])
        key = rotary(key, first_group + c * (CHUNK // GRID_W), CHUNK)
        kv[me, pl.ds(at, CHUNK), 0:HEAD] = key.astype(jnp.bfloat16)
        kv[me, pl.ds(at, CHUNK), HEAD:] = made[:, HEAD : 2 * HEAD]
        lkv[pl.ds(pl.multiple_of(WINDOW + at, WINDOW), CHUNK), :] = made[:, 2 * HEAD :]

    kv_chunk(0)
    loads[5].wait()

    @pl.loop(1, chunks)
    def _(c):
        kv_chunk(c)

    def halo_copy(right):
        src, dst = (rows, 0) if right else (WINDOW, WINDOW + rows)
        return pltpu.make_async_remote_copy(
            src_ref=lkv.at[pl.ds(src, WINDOW)],
            dst_ref=lkv.at[pl.ds(dst, WINDOW)],
            send_sem=halo_send.at[int(right)],
            recv_sem=halo_recv.at[int(right)],
            device_id={"sp": me + (1 if right else -1)},
            device_id_type=MESH,
        )

    def kv_copy(slot, to, sem):
        return pltpu.make_async_remote_copy(
            src_ref=kv.at[slot],
            dst_ref=kv.at[slot],
            send_sem=sem,
            recv_sem=kv_recv.at[slot],
            device_id={"sp": to},
            device_id_type=MESH,
        )

    has_right = me < n_sp - 1
    has_left = me > 0

    @pl.when(has_right)
    def _():
        halo_copy(True).start()

    @pl.when(has_left)
    def _():
        halo_copy(False).start()

    @pl.when(jnp.logical_not(has_left))
    def _():
        lkv[pl.ds(0, WINDOW), :] = jnp.zeros((WINDOW, 2 * HEAD), jnp.bfloat16)

    @pl.when(jnp.logical_not(has_right))
    def _():
        lkv[pl.ds(WINDOW + rows, WINDOW), :] = jnp.zeros((WINDOW, 2 * HEAD), jnp.bfloat16)

    own_sends = ((1, 0), (-1, 1), (2, 2), (-2, 3))
    for step, index in own_sends:
        other = me + step

        @pl.when((other >= 0) & (other < n_sp))
        def _():
            kv_copy(me, other, kv_send.at[index]).start()

    loads[6].wait()
    loads[7].wait()

    @pl.loop(0, chunks)
    def _(c):
        at = pl.multiple_of(c * CHUNK, CHUNK)
        made = dot(normed[pl.ds(at, CHUNK), :], wq[...]).astype(jnp.bfloat16)
        lq_s[pl.ds(at, CHUNK), :] = made[:, 2 * HEAD :]
        for h in range(2):
            x = norm_heads(made[:, h * HEAD : (h + 1) * HEAD].astype(jnp.float32), gq_gain[...])
            x = rotary(x, first_group + c * (CHUNK // GRID_W), CHUNK).astype(jnp.bfloat16)
            for i in range(CHUNK // PIECE):
                u, pos = place(c * (CHUNK // PIECE) + i)
                q_s[u, h, pos] = x[i * PIECE : (i + 1) * PIECE]

    def attend(u, slot, start):
        k = kv[slot, :, 0:HEAD]
        v = with_ones(kv[slot, :, HEAD:])
        for h in range(2):
            q = q_s[u, h].reshape(unit_rows, HEAD)
            s = dot_t(q, k)
            top = jnp.max(s, axis=-1, keepdims=True)
            if start:
                new = top
            else:
                old = m_s[u, h][:, 0:1]
                new = jnp.maximum(old, top)
            p = jnp.exp2((s - new) * (SCALE * LOG2E)).astype(jnp.bfloat16)
            part = dot(p, v)
            if start:
                acc[u, h] = part
            else:
                acc[u, h] = acc[u, h] * jnp.exp2((old - new) * (SCALE * LOG2E)) + part
            m_s[u, h] = jnp.broadcast_to(new, (unit_rows, HEAD))

    @pl.loop(0, units)
    def _(u):
        attend(u, me, True)

    @pl.when(has_left)
    def _():
        halo_copy(True).wait_recv()

    @pl.when(has_right)
    def _():
        halo_copy(False).wait_recv()

    shape = (2 * WINDOW, 3 * WINDOW)
    query_row = lax.broadcasted_iota(jnp.int32, shape, 0)
    query_row = jnp.where(query_row >= WINDOW, query_row - WINDOW, query_row)
    key_col = lax.broadcasted_iota(jnp.int32, shape, 1)
    relative = key_col - WINDOW - query_row
    in_band = (relative <= WINDOW) & (relative >= -WINDOW)
    second = lax.broadcasted_iota(jnp.int32, (2 * WINDOW, 1), 0) >= WINDOW

    @pl.loop(0, rows // WINDOW)
    def _(n):
        at = pl.multiple_of(n * WINDOW, WINDOW)
        q = jnp.concatenate(
            [lq_s[pl.ds(at, WINDOW), 0:HEAD], lq_s[pl.ds(at, WINDOW), HEAD:]], axis=0
        )
        s = dot_t(q, lkv[pl.ds(at, 3 * WINDOW), 0:HEAD]) * SCALE
        key_pos = me * rows + n * WINDOW - WINDOW + key_col
        valid = in_band & (key_pos >= 0) & (key_pos < n_sp * rows)
        s = jnp.where(valid, s, -jnp.inf)
        drain = jnp.where(second, sink[1], sink[0])
        top = jnp.maximum(jnp.max(s, axis=-1, keepdims=True), drain)
        p = jnp.exp(s - top).astype(jnp.bfloat16)
        r = dot(p, with_ones(lkv[pl.ds(at, 3 * WINDOW), HEAD:]))
        r = (r[:, :HEAD] / (r[:, HEAD:] + jnp.exp(drain - top))).astype(jnp.bfloat16)
        for i in range(WINDOW // PIECE):
            u, pos = place(n * (WINDOW // PIECE) + i)
            for h in range(2):
                lo_s[u, pos, :, h * HEAD : (h + 1) * HEAD] = r[
                    h * WINDOW + i * PIECE : h * WINDOW + (i + 1) * PIECE
                ]

    both = jnp.minimum(me, n_sp - 1 - me)
    lean = jnp.where(me < n_sp - 1 - me, 1, -1)

    def block_of(j):
        odd = lax.rem(j, 2)
        paired = me + ((j + 1) // 2) * (2 * odd - 1)
        alone = me + lean * (j - both)
        return jnp.where(j <= 2 * both, paired, alone)

    def onward(slot):
        away = slot - me
        to = jnp.where(away > 0, me - 1, me + 1)
        far = (away >= 2) | (away <= -2)
        return to, far & (to >= 0) & (to < n_sp)

    def arrive(j):
        slot = block_of(j)
        kv_copy(slot, jnp.where(has_left, me - 1, me + 1), fwd_send.at[slot]).wait_recv()
        to, goes = onward(slot)

        @pl.when(goes)
        def _():
            kv_copy(slot, to, fwd_send.at[slot]).start()

        return slot

    @pl.loop(1, n_sp - 1)
    def _(j):
        slot = arrive(j)

        @pl.loop(0, units)
        def _(u):
            attend(u, slot, False)

    def pair_copy(u):
        return pltpu.make_async_remote_copy(
            src_ref=pbuf.at[u, pl.ds((1 - par) * chips, chips)],
            dst_ref=rbuf0.at[u],
            send_sem=r0_send.at[u],
            recv_sem=r0_recv.at[u],
            device_id={"tp": partner},
            device_id_type=MESH,
        )

    def chip_copy(u, k):
        to = lax.rem(chip + k, chips)
        return pltpu.make_async_remote_copy(
            src_ref=sbuf.at[u, k - 1],
            dst_ref=rbuf1.at[u, k - 1],
            send_sem=r1_send.at[u, k - 1],
            recv_sem=r1_recv.at[u, k - 1],
            device_id={"tp": to * 2 + par},
            device_id_type=MESH,
        )

    def spread(u):
        pair_copy(u).wait_recv()
        for k in range(1, chips):
            to = lax.rem(chip + k, chips)
            total = pbuf[u, par * chips + to].astype(jnp.float32) + rbuf0[u, to].astype(
                jnp.float32
            )
            sbuf[u, k - 1] = total.astype(jnp.bfloat16)
            chip_copy(u, k).start()

    last = arrive(n_sp - 1)
    loads[8].wait()
    loads[9].wait()
    tile = 512

    @pl.loop(0, units)
    def _(u):
        attend(u, last, False)
        heads = [(acc[u, h][:, :HEAD] / acc[u, h][:, HEAD:]).astype(jnp.bfloat16) for h in range(2)]
        mixed = jnp.concatenate(heads + [lo_s[u].reshape(unit_rows, 2 * HEAD)], axis=1)
        for i in range(width // tile):
            part = dot(mixed, wo[:, i * tile : (i + 1) * tile]).astype(jnp.bfloat16)
            pbuf[u, :, :, i * tile : (i + 1) * tile] = part.reshape(n_tp, PIECE, tile)
        pair_copy(u).start()

        @pl.when(u > 0)
        def _():
            spread(u - 1)

    spread(units - 1)

    @pl.loop(0, units)
    def _(u):
        total = pbuf[u, par * chips + chip].astype(jnp.float32) + rbuf0[u, chip].astype(
            jnp.float32
        )
        for k in range(1, chips):
            chip_copy(u, k).wait_recv()
            total = total + rbuf1[u, k - 1].astype(jnp.float32)
        out[pl.ds(pl.multiple_of(u * PIECE, PIECE), PIECE), :] = total.astype(jnp.bfloat16)

    @pl.loop(0, units)
    def _(u):
        pair_copy(u).wait_send()
        for k in range(1, chips):
            chip_copy(u, k).wait_send()

    @pl.when(has_right)
    def _():
        halo_copy(True).wait_send()

    @pl.when(has_left)
    def _():
        halo_copy(False).wait_send()

    for step, index in own_sends:
        other = me + step

        @pl.when((other >= 0) & (other < n_sp))
        def _():
            kv_copy(me, other, kv_send.at[index]).wait_send()

    @pl.loop(1, n_sp)
    def _(j):
        slot = block_of(j)
        to, goes = onward(slot)

        @pl.when(goes)
        def _():
            kv_copy(slot, to, fwd_send.at[slot]).wait_send()


def solution(mesh):
    n_sp, n_tp = mesh.shape["sp"], mesh.shape["tp"]

    def shards(
        tokens, norm_gain, gqw, gkw, gvw, gq_gain, gk_gain, lqw, lkw, lvw, sink, gow, low
    ):
        rows, depth = tokens.shape
        width = gow.shape[1]
        units = rows // (n_tp * PIECE)
        unit_rows = n_tp * PIECE
        chips = n_tp // 2
        row_tab, col_tab = rotary_tables(rows * n_sp)
        vmem = pl.BlockSpec(memory_space=pltpu.VMEM)
        hbm = pl.BlockSpec(memory_space=pl.ANY)
        smem = pl.BlockSpec(memory_space=pltpu.SMEM)
        bf16, f32 = jnp.bfloat16, jnp.float32
        dma = pltpu.SemaphoreType.DMA
        return pl.pallas_call(
            functools.partial(kernel, n_sp, n_tp, rows, width),
            out_shape=jax.ShapeDtypeStruct((rows // n_tp, width), bf16),
            in_specs=[
                hbm, vmem, hbm, hbm, hbm, vmem, vmem, hbm, hbm, hbm, smem, hbm, hbm, vmem, vmem
            ],
            out_specs=vmem,
            scratch_shapes=[
                pltpu.VMEM((rows, depth), bf16),
                pltpu.VMEM((rows, depth), bf16),
                pltpu.VMEM((depth, 4 * HEAD), bf16),
                pltpu.VMEM((depth, 4 * HEAD), bf16),
                pltpu.VMEM((4 * HEAD, width), bf16),
                pltpu.VMEM((n_sp, rows, 2 * HEAD), bf16),
                pltpu.VMEM((rows + 2 * WINDOW, 2 * HEAD), bf16),
                pltpu.VMEM((units, 2, n_tp, PIECE, HEAD), bf16),
                pltpu.VMEM((rows, 2 * HEAD), bf16),
                pltpu.VMEM((units, n_tp, PIECE, 2 * HEAD), bf16),
                pltpu.VMEM((units, 2, unit_rows, 2 * HEAD), f32),
                pltpu.VMEM((units, 2, unit_rows, HEAD), f32),
                pltpu.VMEM((units, n_tp, PIECE, width), bf16),
                pltpu.VMEM((units, chips, PIECE, width), bf16),
                pltpu.VMEM((units, chips - 1, PIECE, width), bf16),
                pltpu.VMEM((units, chips - 1, PIECE, width), bf16),
                dma((10,)),
                dma((n_sp,)),
                dma((4,)),
                dma((n_sp,)),
                dma((2,)),
                dma((2,)),
                dma((units,)),
                dma((units,)),
                dma((units, chips - 1)),
                dma((units, chips - 1)),
            ],
            compiler_params=pltpu.CompilerParams(
                collective_id=0, has_side_effects=True, vmem_limit_bytes=60 * 2**20
            ),
            name="attention",
        )(
            tokens, norm_gain.reshape(1, depth), gqw, gkw, gvw,
            gq_gain.reshape(1, HEAD), gk_gain.reshape(1, HEAD), lqw, lkw, lvw,
            sink, gow, low, jnp.asarray(row_tab), jnp.asarray(col_tab),
        )

    in_specs = (
        P("sp", None),
        P(),
        P(None, "tp"),
        P(None, "tp"),
        P(None, "tp"),
        P(),
        P(),
        P(None, "tp"),
        P(None, "tp"),
        P(None, "tp"),
        P("tp"),
        P("tp", None),
        P("tp", None),
    )
    out_specs = P(("sp", "tp"), None)
    return jax.shard_map(shards, mesh=mesh, in_specs=in_specs, out_specs=out_specs, check_vma=False)
```

```python
import functools

import jax
import jax.numpy as jnp
import numpy as np
from jax import lax
from jax.experimental import pallas as pl
from jax.experimental.pallas import tpu as pltpu
from jax.sharding import PartitionSpec as P

HEAD = 128
WINDOW = 128
GRID_W = 64
EPSILON = 1e-06
ROPE_BASE = 10000.0
PIECE = 32
CHUNK = 256
LOG2E = 1.4426950408889634
SCALE = HEAD ** (-0.5)
MESH = pl.DeviceIdType.MESH


def rotary_tables(total_rows):
    half = HEAD // 2
    inverse = (ROPE_BASE ** (-np.arange(0, half, 2, dtype=np.float32) / half)).astype(np.float32)

    def table(count, low):
        angle = np.arange(count, dtype=np.float32)[:, None] * inverse
        cosine = np.cos(angle).astype(np.float32)
        sine = np.sin(angle).astype(np.float32)
        zero = np.zeros((count, half), np.float32)
        cosine = np.concatenate([cosine, cosine], axis=1)
        sine = np.concatenate([-sine, sine], axis=1)
        order = (lambda x: [x, zero]) if low else (lambda x: [zero, x])
        return np.stack(
            [np.concatenate(order(cosine), axis=1), np.concatenate(order(sine), axis=1)]
        )

    return table(total_rows // GRID_W, True), table(GRID_W, False)


def dot(a, b):
    return jnp.dot(a, b, preferred_element_type=jnp.float32)


def dot_t(a, b):
    return lax.dot_general(a, b, (((1,), (1,)), ((), ())), preferred_element_type=jnp.float32)


def with_ones(v):
    return jnp.concatenate([v, jnp.ones((v.shape[0], HEAD), v.dtype)], axis=1)


def kernel(
    n_sp, n_tp, rows, width,
    tokens, gain, gqw, gkw, gvw, gq_gain, gk_gain, lqw, lkw, lvw, sink, gow, low, row_tab, col_tab,
    out,
    tok_v, normed, wkv, wq, wo, kv, lkv, q_s, lq_s, lo_s, acc, m_s, pbuf, rbuf0, sbuf, rbuf1,
    in_sem, kv_recv, kv_send, halo_recv, halo_send, r0_send, r0_recv, r1_send, r1_recv,
):
    me = lax.axis_index("sp")
    tp = lax.axis_index("tp")
    par = lax.rem(tp, 2)
    chip = tp // 2
    chips = n_tp // 2
    units = rows // (n_tp * PIECE)
    unit_rows = n_tp * PIECE
    partner = tp + 1 - 2 * par

    chunks = rows // CHUNK
    loads = []

    def load(src, dst):
        copy = pltpu.make_async_copy(src, dst, in_sem.at[len(loads)])
        copy.start()
        loads.append(copy)

    load(tokens.at[pl.ds(0, CHUNK)], tok_v.at[pl.ds(0, CHUNK)])
    for i, w in enumerate((gkw, gvw, lkw, lvw)):
        load(w, wkv.at[:, pl.ds(i * HEAD, HEAD)])
    load(tokens.at[pl.ds(CHUNK, rows - CHUNK)], tok_v.at[pl.ds(CHUNK, rows - CHUNK)])
    load(gqw, wq.at[:, pl.ds(0, 2 * HEAD)])
    load(lqw, wq.at[:, pl.ds(2 * HEAD, 2 * HEAD)])
    load(gow, wo.at[pl.ds(0, 2 * HEAD)])
    load(low, wo.at[pl.ds(2 * HEAD, 2 * HEAD)])

    barrier = pltpu.get_barrier_semaphore()
    for step in (-1, 1):
        other = me + step

        @pl.when((other >= 0) & (other < n_sp))
        def _():
            pl.semaphore_signal(barrier, inc=1, device_id={"sp": other}, device_id_type=MESH)

    pl.semaphore_signal(barrier, inc=1, device_id={"tp": partner}, device_id_type=MESH)
    for k in range(1, chips):
        peer = lax.rem(chip + k, chips) * 2 + par
        pl.semaphore_signal(barrier, inc=1, device_id={"tp": peer}, device_id_type=MESH)
    near = jnp.minimum(me, 1) + jnp.minimum(n_sp - 1 - me, 1)
    pl.semaphore_wait(barrier, near + chips)

    def norm_heads(x, head_gain):
        return x * lax.rsqrt(jnp.mean(x * x, axis=-1, keepdims=True) + EPSILON) * head_gain

    def rotary(x, group, count):
        def tiled(k):
            return jnp.concatenate(
                [row_tab[k, pl.ds(group + i, 1), :] + col_tab[k] for i in range(count // GRID_W)],
                axis=0,
            )

        lane = lax.broadcasted_iota(jnp.int32, x.shape, 1)
        quarter = HEAD // 4
        first = lax.rem(lane, 2 * quarter) < quarter
        turned = jnp.where(
            first, pltpu.roll(x, HEAD - quarter, 1), pltpu.roll(x, quarter, 1)
        )
        return x * tiled(0) + turned * tiled(1)

    def place(g):
        t = g // units
        return lax.rem(g, units), lax.rem(t, 2) * chips + t // 2

    first_group = me * (rows // GRID_W)

    has_right = me < n_sp - 1
    has_left = me > 0
    order = [0] + [chunks - 1] * (chunks > 1) + list(range(1, chunks - 1))

    def halo_copy(right):
        src, dst = (rows, 0) if right else (WINDOW, WINDOW + rows)
        return pltpu.make_async_remote_copy(
            src_ref=lkv.at[pl.ds(src, WINDOW)],
            dst_ref=lkv.at[pl.ds(dst, WINDOW)],
            send_sem=halo_send.at[int(right)],
            recv_sem=halo_recv.at[int(right)],
            device_id={"sp": me + (1 if right else -1)},
            device_id_type=MESH,
        )

    def kv_copy(slot, piece, right):
        part = kv.at[slot, pl.ds(piece * CHUNK, CHUNK)]
        return pltpu.make_async_remote_copy(
            src_ref=part,
            dst_ref=part,
            send_sem=kv_send.at[slot, piece, int(right)],
            recv_sem=kv_recv.at[slot, piece],
            device_id={"sp": me + (1 if right else -1)},
            device_id_type=MESH,
        )

    @pl.when(jnp.logical_not(has_left))
    def _():
        lkv[pl.ds(0, WINDOW), :] = jnp.zeros((WINDOW, 2 * HEAD), jnp.bfloat16)

    @pl.when(jnp.logical_not(has_right))
    def _():
        lkv[pl.ds(WINDOW + rows, WINDOW), :] = jnp.zeros((WINDOW, 2 * HEAD), jnp.bfloat16)

    loads[0].wait()
    for i in range(1, 5):
        loads[i].wait()

    def kv_chunk(c):
        at = pl.multiple_of(c * CHUNK, CHUNK)
        wide = tok_v[pl.ds(at, CHUNK), :].astype(jnp.float32)
        mean = jnp.mean(wide * wide, axis=-1, keepdims=True)
        scaled = (wide * lax.rsqrt(mean + EPSILON) * gain[...]).astype(jnp.bfloat16)
        normed[pl.ds(at, CHUNK), :] = scaled
        made = dot(scaled, wkv[...]).astype(jnp.bfloat16)
        key = norm_heads(made[:, :HEAD].astype(jnp.float32), gk_gain[...])
        key = rotary(key, first_group + c * (CHUNK // GRID_W), CHUNK)
        kv[me, pl.ds(at, CHUNK), 0:HEAD] = key.astype(jnp.bfloat16)
        kv[me, pl.ds(at, CHUNK), HEAD:] = made[:, HEAD : 2 * HEAD]
        lkv[pl.ds(pl.multiple_of(WINDOW + at, WINDOW), CHUNK), :] = made[:, 2 * HEAD :]

    for step, c in enumerate(order):
        if step == 1:
            loads[5].wait()
        kv_chunk(c)

        @pl.when(has_right)
        def _():
            if c == chunks - 1:
                halo_copy(True).start()
            kv_copy(me, c, True).start()

        @pl.when(has_left)
        def _():
            if c == 0:
                halo_copy(False).start()
            kv_copy(me, c, False).start()

    def relay(k, piece):
        for right in (True, False):
            slot = me + k if right else me - k
            here = (slot < n_sp) if right else (slot >= 0)

            @pl.when(here)
            def _():
                kv_copy(slot, piece, not right).wait_recv()

                @pl.when(has_left if right else has_right)
                def _():
                    kv_copy(slot, piece, not right).start()

    loads[6].wait()
    loads[7].wait()

    @pl.loop(0, chunks)
    def _(c):
        at = pl.multiple_of(c * CHUNK, CHUNK)
        made = dot(normed[pl.ds(at, CHUNK), :], wq[...]).astype(jnp.bfloat16)
        lq_s[pl.ds(at, CHUNK), :] = made[:, 2 * HEAD :]
        for h in range(2):
            x = norm_heads(made[:, h * HEAD : (h + 1) * HEAD].astype(jnp.float32), gq_gain[...])
            x = rotary(x, first_group + c * (CHUNK // GRID_W), CHUNK).astype(jnp.bfloat16)
            for i in range(CHUNK // PIECE):
                u, pos = place(c * (CHUNK // PIECE) + i)
                q_s[u, h, pos] = x[i * PIECE : (i + 1) * PIECE]

    def attend(u, slot, start):
        k = kv[slot, :, 0:HEAD]
        v = with_ones(kv[slot, :, HEAD:])
        for h in range(2):
            q = q_s[u, h].reshape(unit_rows, HEAD)
            s = dot_t(q, k)
            top = jnp.max(s, axis=-1, keepdims=True)
            if start:
                new = top
            else:
                old = m_s[u, h][:, 0:1]
                new = jnp.maximum(old, top)
            p = jnp.exp2((s - new) * (SCALE * LOG2E)).astype(jnp.bfloat16)
            part = dot(p, v)
            if start:
                acc[u, h] = part
            else:
                acc[u, h] = acc[u, h] * jnp.exp2((old - new) * (SCALE * LOG2E)) + part
            m_s[u, h] = jnp.broadcast_to(new, (unit_rows, HEAD))

    @pl.loop(0, units)
    def _(u):
        attend(u, me, True)

    for piece in order[:2]:
        relay(1, piece)

    @pl.when(has_left)
    def _():
        halo_copy(True).wait_recv()

    @pl.when(has_right)
    def _():
        halo_copy(False).wait_recv()

    shape = (2 * WINDOW, 3 * WINDOW)
    query_row = lax.broadcasted_iota(jnp.int32, shape, 0)
    query_row = jnp.where(query_row >= WINDOW, query_row - WINDOW, query_row)
    key_col = lax.broadcasted_iota(jnp.int32, shape, 1)
    relative = key_col - WINDOW - query_row
    in_band = (relative <= WINDOW) & (relative >= -WINDOW)
    second = lax.broadcasted_iota(jnp.int32, (2 * WINDOW, 1), 0) >= WINDOW

    @pl.loop(0, rows // WINDOW)
    def _(n):
        at = pl.multiple_of(n * WINDOW, WINDOW)
        q = jnp.concatenate(
            [lq_s[pl.ds(at, WINDOW), 0:HEAD], lq_s[pl.ds(at, WINDOW), HEAD:]], axis=0
        )
        s = dot_t(q, lkv[pl.ds(at, 3 * WINDOW), 0:HEAD]) * SCALE
        key_pos = me * rows + n * WINDOW - WINDOW + key_col
        valid = in_band & (key_pos >= 0) & (key_pos < n_sp * rows)
        s = jnp.where(valid, s, -jnp.inf)
        drain = jnp.where(second, sink[1], sink[0])
        top = jnp.maximum(jnp.max(s, axis=-1, keepdims=True), drain)
        p = jnp.exp(s - top).astype(jnp.bfloat16)
        r = dot(p, with_ones(lkv[pl.ds(at, 3 * WINDOW), HEAD:]))
        r = (r[:, :HEAD] / (r[:, HEAD:] + jnp.exp(drain - top))).astype(jnp.bfloat16)
        for i in range(WINDOW // PIECE):
            u, pos = place(n * (WINDOW // PIECE) + i)
            for h in range(2):
                lo_s[u, pos, :, h * HEAD : (h + 1) * HEAD] = r[
                    h * WINDOW + i * PIECE : h * WINDOW + (i + 1) * PIECE
                ]

    both = jnp.minimum(me, n_sp - 1 - me)
    lean = jnp.where(me < n_sp - 1 - me, 1, -1)

    def block_of(j):
        odd = lax.rem(j, 2)
        paired = me + ((j + 1) // 2) * (2 * odd - 1)
        alone = me + lean * (j - both)
        return jnp.where(j <= 2 * both, paired, alone)

    for piece in order[2:]:
        relay(1, piece)

    @pl.loop(1, n_sp - 1)
    def _(j):
        slot = block_of(j)
        alone = j > 2 * both
        k = jnp.where(alone, j - both, (j + 1) // 2)
        first = alone | (lax.rem(j, 2) == 1)
        final = alone | (lax.rem(j, 2) == 0)

        @pl.loop(0, units)
        def _(u):
            attend(u, slot, False)

        @pl.when(first)
        def _():
            relay(k + 1, order[0])

        @pl.when(final)
        def _():
            for piece in order[1:]:
                relay(k + 1, piece)

    def pair_copy(u):
        return pltpu.make_async_remote_copy(
            src_ref=pbuf.at[u, pl.ds((1 - par) * chips, chips)],
            dst_ref=rbuf0.at[u],
            send_sem=r0_send.at[u],
            recv_sem=r0_recv.at[u],
            device_id={"tp": partner},
            device_id_type=MESH,
        )

    def chip_copy(u, k):
        to = lax.rem(chip + k, chips)
        return pltpu.make_async_remote_copy(
            src_ref=sbuf.at[u, k - 1],
            dst_ref=rbuf1.at[u, k - 1],
            send_sem=r1_send.at[u, k - 1],
            recv_sem=r1_recv.at[u, k - 1],
            device_id={"tp": to * 2 + par},
            device_id_type=MESH,
        )

    def spread(u):
        pair_copy(u).wait_recv()
        for k in range(1, chips):
            to = lax.rem(chip + k, chips)
            total = pbuf[u, par * chips + to].astype(jnp.float32) + rbuf0[u, to].astype(
                jnp.float32
            )
            sbuf[u, k - 1] = total.astype(jnp.bfloat16)
            chip_copy(u, k).start()

    last = block_of(n_sp - 1)
    loads[8].wait()
    loads[9].wait()
    tile = 512

    @pl.loop(0, units)
    def _(u):
        attend(u, last, False)
        heads = [(acc[u, h][:, :HEAD] / acc[u, h][:, HEAD:]).astype(jnp.bfloat16) for h in range(2)]
        mixed = jnp.concatenate(heads + [lo_s[u].reshape(unit_rows, 2 * HEAD)], axis=1)
        for i in range(width // tile):
            part = dot(mixed, wo[:, i * tile : (i + 1) * tile]).astype(jnp.bfloat16)
            pbuf[u, :, :, i * tile : (i + 1) * tile] = part.reshape(n_tp, PIECE, tile)
        pair_copy(u).start()

        @pl.when(u > 0)
        def _():
            spread(u - 1)

    spread(units - 1)

    @pl.loop(0, units)
    def _(u):
        total = pbuf[u, par * chips + chip].astype(jnp.float32) + rbuf0[u, chip].astype(
            jnp.float32
        )
        for k in range(1, chips):
            chip_copy(u, k).wait_recv()
            total = total + rbuf1[u, k - 1].astype(jnp.float32)
        out[pl.ds(pl.multiple_of(u * PIECE, PIECE), PIECE), :] = total.astype(jnp.bfloat16)

    @pl.loop(0, units)
    def _(u):
        pair_copy(u).wait_send()
        for k in range(1, chips):
            chip_copy(u, k).wait_send()

    @pl.when(has_right)
    def _():
        halo_copy(True).wait_send()

    @pl.when(has_left)
    def _():
        halo_copy(False).wait_send()

    @pl.loop(0, n_sp)
    def _(slot):
        @pl.when((slot <= me) & has_right)
        def _():
            for piece in order:
                kv_copy(slot, piece, True).wait_send()

        @pl.when((slot >= me) & has_left)
        def _():
            for piece in order:
                kv_copy(slot, piece, False).wait_send()


def solution(mesh):
    n_sp, n_tp = mesh.shape["sp"], mesh.shape["tp"]

    def shards(
        tokens, norm_gain, gqw, gkw, gvw, gq_gain, gk_gain, lqw, lkw, lvw, sink, gow, low
    ):
        rows, depth = tokens.shape
        width = gow.shape[1]
        units = rows // (n_tp * PIECE)
        unit_rows = n_tp * PIECE
        chips = n_tp // 2
        row_tab, col_tab = rotary_tables(rows * n_sp)
        vmem = pl.BlockSpec(memory_space=pltpu.VMEM)
        hbm = pl.BlockSpec(memory_space=pl.ANY)
        smem = pl.BlockSpec(memory_space=pltpu.SMEM)
        bf16, f32 = jnp.bfloat16, jnp.float32
        dma = pltpu.SemaphoreType.DMA
        return pl.pallas_call(
            functools.partial(kernel, n_sp, n_tp, rows, width),
            out_shape=jax.ShapeDtypeStruct((rows // n_tp, width), bf16),
            in_specs=[
                hbm, vmem, hbm, hbm, hbm, vmem, vmem, hbm, hbm, hbm, smem, hbm, hbm, vmem, vmem
            ],
            out_specs=vmem,
            scratch_shapes=[
                pltpu.VMEM((rows, depth), bf16),
                pltpu.VMEM((rows, depth), bf16),
                pltpu.VMEM((depth, 4 * HEAD), bf16),
                pltpu.VMEM((depth, 4 * HEAD), bf16),
                pltpu.VMEM((4 * HEAD, width), bf16),
                pltpu.VMEM((n_sp, rows, 2 * HEAD), bf16),
                pltpu.VMEM((rows + 2 * WINDOW, 2 * HEAD), bf16),
                pltpu.VMEM((units, 2, n_tp, PIECE, HEAD), bf16),
                pltpu.VMEM((rows, 2 * HEAD), bf16),
                pltpu.VMEM((units, n_tp, PIECE, 2 * HEAD), bf16),
                pltpu.VMEM((units, 2, unit_rows, 2 * HEAD), f32),
                pltpu.VMEM((units, 2, unit_rows, HEAD), f32),
                pltpu.VMEM((units, n_tp, PIECE, width), bf16),
                pltpu.VMEM((units, chips, PIECE, width), bf16),
                pltpu.VMEM((units, chips - 1, PIECE, width), bf16),
                pltpu.VMEM((units, chips - 1, PIECE, width), bf16),
                dma((10,)),
                dma((n_sp, rows // CHUNK)),
                dma((n_sp, rows // CHUNK, 2)),
                dma((2,)),
                dma((2,)),
                dma((units,)),
                dma((units,)),
                dma((units, chips - 1)),
                dma((units, chips - 1)),
            ],
            compiler_params=pltpu.CompilerParams(
                collective_id=0, has_side_effects=True, vmem_limit_bytes=60 * 2**20
            ),
            name="attention",
        )(
            tokens, norm_gain.reshape(1, depth), gqw, gkw, gvw,
            gq_gain.reshape(1, HEAD), gk_gain.reshape(1, HEAD), lqw, lkw, lvw,
            sink, gow, low, jnp.asarray(row_tab), jnp.asarray(col_tab),
        )

    in_specs = (
        P("sp", None),
        P(),
        P(None, "tp"),
        P(None, "tp"),
        P(None, "tp"),
        P(),
        P(),
        P(None, "tp"),
        P(None, "tp"),
        P(None, "tp"),
        P("tp"),
        P("tp", None),
        P("tp", None),
    )
    out_specs = P(("sp", "tp"), None)
    return jax.shard_map(shards, mesh=mesh, in_specs=in_specs, out_specs=out_specs, check_vma=False)
```

```python
import functools

import jax
import jax.numpy as jnp
import numpy as np
from jax import lax
from jax.experimental import pallas as pl
from jax.experimental.pallas import tpu as pltpu
from jax.sharding import PartitionSpec as P

HEAD = 128
WINDOW = 128
GRID_W = 64
EPSILON = 1e-06
ROPE_BASE = 10000.0
PIECE = 32
CHUNK = 256
LOG2E = 1.4426950408889634
SCALE = HEAD ** (-0.5)
MESH = pl.DeviceIdType.MESH


def rotary_tables(total_rows):
    half = HEAD // 2
    inverse = (ROPE_BASE ** (-np.arange(0, half, 2, dtype=np.float32) / half)).astype(np.float32)

    def table(count, low):
        angle = np.arange(count, dtype=np.float32)[:, None] * inverse
        cosine = np.cos(angle).astype(np.float32)
        sine = np.sin(angle).astype(np.float32)
        zero = np.zeros((count, half), np.float32)
        cosine = np.concatenate([cosine, cosine], axis=1)
        sine = np.concatenate([-sine, sine], axis=1)
        order = (lambda x: [x, zero]) if low else (lambda x: [zero, x])
        return np.stack(
            [np.concatenate(order(cosine), axis=1), np.concatenate(order(sine), axis=1)]
        )

    return table(total_rows // GRID_W, True), table(GRID_W, False)


def dot(a, b):
    return jnp.dot(a, b, preferred_element_type=jnp.float32)


def dot_t(a, b):
    return lax.dot_general(a, b, (((1,), (1,)), ((), ())), preferred_element_type=jnp.float32)


def with_ones(v):
    return jnp.concatenate([v, jnp.ones((v.shape[0], HEAD), v.dtype)], axis=1)


def kernel(
    n_sp, n_tp, rows, width,
    tokens, gain, gqw, gkw, gvw, gq_gain, gk_gain, lqw, lkw, lvw, sink, gow, low, row_tab, col_tab,
    out,
    tok_v, normed, wkv, wq, wo, kv, lkv, q_s, lq_s, lo_s, acc, m_s, pbuf, rbuf0, sbuf1, rbuf1, sbuf2, rbuf2,
    in_sem, kv_recv, kv_send, halo_recv, halo_send, r0_send, r0_recv, r1_send, r1_recv,
):
    me = lax.axis_index("sp")
    tp = lax.axis_index("tp")
    par = lax.rem(tp, 2)
    chip = tp // 2
    chips = n_tp // 2
    units = rows // (n_tp * PIECE)
    unit_rows = n_tp * PIECE
    partner = tp + 1 - 2 * par

    def facing(k):
        low_bit, high_bit = lax.rem(chip, 2), chip // 2
        if k & 1:
            low_bit = 1 - low_bit
        if k & 2:
            high_bit = 1 - high_bit
        return high_bit * 2 + low_bit


    chunks = rows // CHUNK
    loads = []

    def load(src, dst):
        copy = pltpu.make_async_copy(src, dst, in_sem.at[len(loads)])
        copy.start()
        loads.append(copy)

    load(tokens.at[pl.ds(0, CHUNK)], tok_v.at[pl.ds(0, CHUNK)])
    for i, w in enumerate((gkw, gvw, lkw, lvw)):
        load(w, wkv.at[:, pl.ds(i * HEAD, HEAD)])
    load(tokens.at[pl.ds(CHUNK, rows - CHUNK)], tok_v.at[pl.ds(CHUNK, rows - CHUNK)])
    load(gqw, wq.at[:, pl.ds(0, 2 * HEAD)])
    load(lqw, wq.at[:, pl.ds(2 * HEAD, 2 * HEAD)])
    load(gow, wo.at[pl.ds(0, 2 * HEAD)])
    load(low, wo.at[pl.ds(2 * HEAD, 2 * HEAD)])

    barrier = pltpu.get_barrier_semaphore()
    for step in (-1, 1):
        other = me + step

        @pl.when((other >= 0) & (other < n_sp))
        def _():
            pl.semaphore_signal(barrier, inc=1, device_id={"sp": other}, device_id_type=MESH)

    pl.semaphore_signal(barrier, inc=1, device_id={"tp": partner}, device_id_type=MESH)
    for k in (1, 2):
        pl.semaphore_signal(
            barrier, inc=1, device_id={"tp": facing(k) * 2 + par}, device_id_type=MESH
        )
    near = jnp.minimum(me, 1) + jnp.minimum(n_sp - 1 - me, 1)

    def norm_heads(x, head_gain):
        return x * lax.rsqrt(jnp.mean(x * x, axis=-1, keepdims=True) + EPSILON) * head_gain

    def rotary(x, group, count):
        def tiled(k):
            return jnp.concatenate(
                [row_tab[k, pl.ds(group + i, 1), :] + col_tab[k] for i in range(count // GRID_W)],
                axis=0,
            )

        lane = lax.broadcasted_iota(jnp.int32, x.shape, 1)
        quarter = HEAD // 4
        first = lax.rem(lane, 2 * quarter) < quarter
        turned = jnp.where(
            first, pltpu.roll(x, HEAD - quarter, 1), pltpu.roll(x, quarter, 1)
        )
        return x * tiled(0) + turned * tiled(1)

    def place(g):
        t = g // units
        return lax.rem(g, units), lax.rem(t, 2) * chips + t // 2

    first_group = me * (rows // GRID_W)

    has_right = me < n_sp - 1
    has_left = me > 0
    order = [0] + [chunks - 1] * (chunks > 1) + list(range(1, chunks - 1))

    def halo_copy(right):
        src, dst = (rows, 0) if right else (WINDOW, WINDOW + rows)
        return pltpu.make_async_remote_copy(
            src_ref=lkv.at[pl.ds(src, WINDOW)],
            dst_ref=lkv.at[pl.ds(dst, WINDOW)],
            send_sem=halo_send.at[int(right)],
            recv_sem=halo_recv.at[int(right)],
            device_id={"sp": me + (1 if right else -1)},
            device_id_type=MESH,
        )

    def kv_copy(slot, piece, right):
        part = kv.at[slot, pl.ds(piece * CHUNK, CHUNK)]
        return pltpu.make_async_remote_copy(
            src_ref=part,
            dst_ref=part,
            send_sem=kv_send.at[slot, piece, int(right)],
            recv_sem=kv_recv.at[slot, piece],
            device_id={"sp": me + (1 if right else -1)},
            device_id_type=MESH,
        )

    @pl.when(jnp.logical_not(has_left))
    def _():
        lkv[pl.ds(0, WINDOW), :] = jnp.zeros((WINDOW, 2 * HEAD), jnp.bfloat16)

    @pl.when(jnp.logical_not(has_right))
    def _():
        lkv[pl.ds(WINDOW + rows, WINDOW), :] = jnp.zeros((WINDOW, 2 * HEAD), jnp.bfloat16)

    loads[0].wait()
    for i in range(1, 5):
        loads[i].wait()

    def kv_chunk(c):
        at = pl.multiple_of(c * CHUNK, CHUNK)
        wide = tok_v[pl.ds(at, CHUNK), :].astype(jnp.float32)
        mean = jnp.mean(wide * wide, axis=-1, keepdims=True)
        scaled = (wide * lax.rsqrt(mean + EPSILON) * gain[...]).astype(jnp.bfloat16)
        normed[pl.ds(at, CHUNK), :] = scaled
        made = dot(scaled, wkv[...]).astype(jnp.bfloat16)
        key = norm_heads(made[:, :HEAD].astype(jnp.float32), gk_gain[...])
        key = rotary(key, first_group + c * (CHUNK // GRID_W), CHUNK)
        kv[me, pl.ds(at, CHUNK), 0:HEAD] = key.astype(jnp.bfloat16)
        kv[me, pl.ds(at, CHUNK), HEAD:] = made[:, HEAD : 2 * HEAD]
        lkv[pl.ds(pl.multiple_of(WINDOW + at, WINDOW), CHUNK), :] = made[:, 2 * HEAD :]

    for step, c in enumerate(order):
        if step == 1:
            loads[5].wait()
        kv_chunk(c)
        if step == 0:
            pl.semaphore_wait(barrier, near + 3)

        @pl.when(has_right)
        def _():
            if c == chunks - 1:
                halo_copy(True).start()
            kv_copy(me, c, True).start()

        @pl.when(has_left)
        def _():
            if c == 0:
                halo_copy(False).start()
            kv_copy(me, c, False).start()

    def relay(k, piece):
        for right in (True, False):
            slot = me + k if right else me - k
            here = (slot < n_sp) if right else (slot >= 0)

            @pl.when(here)
            def _():
                kv_copy(slot, piece, not right).wait_recv()

                @pl.when(has_left if right else has_right)
                def _():
                    kv_copy(slot, piece, not right).start()

    loads[6].wait()
    loads[7].wait()

    @pl.loop(0, chunks)
    def _(c):
        at = pl.multiple_of(c * CHUNK, CHUNK)
        made = dot(normed[pl.ds(at, CHUNK), :], wq[...]).astype(jnp.bfloat16)
        lq_s[pl.ds(at, CHUNK), :] = made[:, 2 * HEAD :]
        for h in range(2):
            x = norm_heads(made[:, h * HEAD : (h + 1) * HEAD].astype(jnp.float32), gq_gain[...])
            x = rotary(x, first_group + c * (CHUNK // GRID_W), CHUNK).astype(jnp.bfloat16)
            for i in range(CHUNK // PIECE):
                u, pos = place(c * (CHUNK // PIECE) + i)
                q_s[u, h, pos] = x[i * PIECE : (i + 1) * PIECE]

    def attend(u, slot, start):
        k = kv[slot, :, 0:HEAD]
        v = with_ones(kv[slot, :, HEAD:])
        for h in range(2):
            q = q_s[u, h].reshape(unit_rows, HEAD)
            s = dot_t(q, k)
            top = jnp.max(s, axis=-1, keepdims=True)
            if start:
                new = top
            else:
                old = m_s[u, h][:, 0:1]
                new = jnp.maximum(old, top)
            p = jnp.exp2((s - new) * (SCALE * LOG2E)).astype(jnp.bfloat16)
            part = dot(p, v)
            if start:
                acc[u, h] = part
            else:
                acc[u, h] = acc[u, h] * jnp.exp2((old - new) * (SCALE * LOG2E)) + part
            m_s[u, h] = jnp.broadcast_to(new, (unit_rows, HEAD))

    @pl.loop(0, units)
    def _(u):
        attend(u, me, True)

    for piece in order[:2]:
        relay(1, piece)

    @pl.when(has_left)
    def _():
        halo_copy(True).wait_recv()

    @pl.when(has_right)
    def _():
        halo_copy(False).wait_recv()

    shape = (2 * WINDOW, 3 * WINDOW)
    query_row = lax.broadcasted_iota(jnp.int32, shape, 0)
    query_row = jnp.where(query_row >= WINDOW, query_row - WINDOW, query_row)
    key_col = lax.broadcasted_iota(jnp.int32, shape, 1)
    relative = key_col - WINDOW - query_row
    in_band = (relative <= WINDOW) & (relative >= -WINDOW)
    second = lax.broadcasted_iota(jnp.int32, (2 * WINDOW, 1), 0) >= WINDOW

    @pl.loop(0, rows // WINDOW)
    def _(n):
        at = pl.multiple_of(n * WINDOW, WINDOW)
        q = jnp.concatenate(
            [lq_s[pl.ds(at, WINDOW), 0:HEAD], lq_s[pl.ds(at, WINDOW), HEAD:]], axis=0
        )
        s = dot_t(q, lkv[pl.ds(at, 3 * WINDOW), 0:HEAD]) * SCALE
        key_pos = me * rows + n * WINDOW - WINDOW + key_col
        valid = in_band & (key_pos >= 0) & (key_pos < n_sp * rows)
        s = jnp.where(valid, s, -jnp.inf)
        drain = jnp.where(second, sink[1], sink[0])
        top = jnp.maximum(jnp.max(s, axis=-1, keepdims=True), drain)
        p = jnp.exp(s - top).astype(jnp.bfloat16)
        r = dot(p, with_ones(lkv[pl.ds(at, 3 * WINDOW), HEAD:]))
        r = (r[:, :HEAD] / (r[:, HEAD:] + jnp.exp(drain - top))).astype(jnp.bfloat16)
        for i in range(WINDOW // PIECE):
            u, pos = place(n * (WINDOW // PIECE) + i)
            for h in range(2):
                lo_s[u, pos, :, h * HEAD : (h + 1) * HEAD] = r[
                    h * WINDOW + i * PIECE : h * WINDOW + (i + 1) * PIECE
                ]

    both = jnp.minimum(me, n_sp - 1 - me)
    lean = jnp.where(me < n_sp - 1 - me, 1, -1)

    def block_of(j):
        odd = lax.rem(j, 2)
        paired = me + ((j + 1) // 2) * (2 * odd - 1)
        alone = me + lean * (j - both)
        return jnp.where(j <= 2 * both, paired, alone)

    for piece in order[2:]:
        relay(1, piece)

    @pl.loop(1, n_sp - 1)
    def _(j):
        slot = block_of(j)
        alone = j > 2 * both
        k = jnp.where(alone, j - both, (j + 1) // 2)
        first = alone | (lax.rem(j, 2) == 1)
        final = alone | (lax.rem(j, 2) == 0)

        @pl.loop(0, units)
        def _(u):
            attend(u, slot, False)

        @pl.when(first)
        def _():
            relay(k + 1, order[0])

        @pl.when(final)
        def _():
            for piece in order[1:]:
                relay(k + 1, piece)

    def pair_copy(u):
        return pltpu.make_async_remote_copy(
            src_ref=pbuf.at[u, pl.ds((1 - par) * chips, chips)],
            dst_ref=rbuf0.at[u],
            send_sem=r0_send.at[u],
            recv_sem=r0_recv.at[u],
            device_id={"tp": partner},
            device_id_type=MESH,
        )

    half = width // 2
    columns = (slice(0, half), slice(half, width))

    def chip_copy(u, stage, way):
        src, dst = (sbuf1, rbuf1) if stage == 0 else (sbuf2, rbuf2)
        peer = facing(1 if stage == way else 2)
        return pltpu.make_async_remote_copy(
            src_ref=src.at[u, way],
            dst_ref=dst.at[u, way],
            send_sem=r1_send.at[u, stage, way],
            recv_sem=r1_recv.at[u, stage, way],
            device_id={"tp": peer * 2 + par},
            device_id_type=MESH,
        )

    def paired(u, to, way):
        return pbuf[u, par * chips + to, :, columns[way]].astype(jnp.float32) + rbuf0[
            u, to, :, columns[way]
        ].astype(jnp.float32)

    def spread(u):
        pair_copy(u).wait_recv()
        for way in range(2):
            sbuf1[u, way, 0] = paired(u, facing(1 + way), way).astype(jnp.bfloat16)
            sbuf1[u, way, 1] = paired(u, facing(3), way).astype(jnp.bfloat16)
            chip_copy(u, 0, way).start()

    def pass_on(u):
        for way in range(2):
            chip_copy(u, 0, way).wait_recv()
            total = paired(u, facing(2 - way), way) + rbuf1[u, way, 1].astype(jnp.float32)
            sbuf2[u, way] = total.astype(jnp.bfloat16)
            chip_copy(u, 1, way).start()

    last = block_of(n_sp - 1)
    loads[8].wait()
    loads[9].wait()
    tile = 512

    @pl.loop(0, units)
    def _(u):
        attend(u, last, False)
        heads = [(acc[u, h][:, :HEAD] / acc[u, h][:, HEAD:]).astype(jnp.bfloat16) for h in range(2)]
        mixed = jnp.concatenate(heads + [lo_s[u].reshape(unit_rows, 2 * HEAD)], axis=1)
        for i in range(width // tile):
            part = dot(mixed, wo[:, i * tile : (i + 1) * tile]).astype(jnp.bfloat16)
            pbuf[u, :, :, i * tile : (i + 1) * tile] = part.reshape(n_tp, PIECE, tile)
        pair_copy(u).start()

        @pl.when(u > 0)
        def _():
            spread(u - 1)

    spread(units - 1)

    @pl.loop(0, units)
    def _(u):
        pass_on(u)

    @pl.loop(0, units)
    def _(u):
        at = pl.ds(pl.multiple_of(u * PIECE, PIECE), PIECE)
        for way in range(2):
            chip_copy(u, 1, way).wait_recv()
            total = paired(u, chip, way) + rbuf1[u, way, 0].astype(jnp.float32)
            total = total + rbuf2[u, way].astype(jnp.float32)
            out[at, columns[way]] = total.astype(jnp.bfloat16)

    @pl.loop(0, units)
    def _(u):
        pair_copy(u).wait_send()
        for stage in range(2):
            for way in range(2):
                chip_copy(u, stage, way).wait_send()

    @pl.when(has_right)
    def _():
        halo_copy(True).wait_send()

    @pl.when(has_left)
    def _():
        halo_copy(False).wait_send()

    @pl.loop(0, n_sp)
    def _(slot):
        @pl.when((slot <= me) & has_right)
        def _():
            for piece in order:
                kv_copy(slot, piece, True).wait_send()

        @pl.when((slot >= me) & has_left)
        def _():
            for piece in order:
                kv_copy(slot, piece, False).wait_send()


def solution(mesh):
    n_sp, n_tp = mesh.shape["sp"], mesh.shape["tp"]

    def shards(
        tokens, norm_gain, gqw, gkw, gvw, gq_gain, gk_gain, lqw, lkw, lvw, sink, gow, low
    ):
        rows, depth = tokens.shape
        width = gow.shape[1]
        units = rows // (n_tp * PIECE)
        unit_rows = n_tp * PIECE
        chips = n_tp // 2
        row_tab, col_tab = rotary_tables(rows * n_sp)
        vmem = pl.BlockSpec(memory_space=pltpu.VMEM)
        hbm = pl.BlockSpec(memory_space=pl.ANY)
        smem = pl.BlockSpec(memory_space=pltpu.SMEM)
        bf16, f32 = jnp.bfloat16, jnp.float32
        dma = pltpu.SemaphoreType.DMA
        return pl.pallas_call(
            functools.partial(kernel, n_sp, n_tp, rows, width),
            out_shape=jax.ShapeDtypeStruct((rows // n_tp, width), bf16),
            in_specs=[
                hbm, vmem, hbm, hbm, hbm, vmem, vmem, hbm, hbm, hbm, smem, hbm, hbm, vmem, vmem
            ],
            out_specs=vmem,
            scratch_shapes=[
                pltpu.VMEM((rows, depth), bf16),
                pltpu.VMEM((rows, depth), bf16),
                pltpu.VMEM((depth, 4 * HEAD), bf16),
                pltpu.VMEM((depth, 4 * HEAD), bf16),
                pltpu.VMEM((4 * HEAD, width), bf16),
                pltpu.VMEM((n_sp, rows, 2 * HEAD), bf16),
                pltpu.VMEM((rows + 2 * WINDOW, 2 * HEAD), bf16),
                pltpu.VMEM((units, 2, n_tp, PIECE, HEAD), bf16),
                pltpu.VMEM((rows, 2 * HEAD), bf16),
                pltpu.VMEM((units, n_tp, PIECE, 2 * HEAD), bf16),
                pltpu.VMEM((units, 2, unit_rows, 2 * HEAD), f32),
                pltpu.VMEM((units, 2, unit_rows, HEAD), f32),
                pltpu.VMEM((units, n_tp, PIECE, width), bf16),
                pltpu.VMEM((units, chips, PIECE, width), bf16),
                pltpu.VMEM((units, 2, 2, PIECE, width // 2), bf16),
                pltpu.VMEM((units, 2, 2, PIECE, width // 2), bf16),
                pltpu.VMEM((units, 2, PIECE, width // 2), bf16),
                pltpu.VMEM((units, 2, PIECE, width // 2), bf16),
                dma((10,)),
                dma((n_sp, rows // CHUNK)),
                dma((n_sp, rows // CHUNK, 2)),
                dma((2,)),
                dma((2,)),
                dma((units,)),
                dma((units,)),
                dma((units, 2, 2)),
                dma((units, 2, 2)),
            ],
            compiler_params=pltpu.CompilerParams(
                collective_id=0, has_side_effects=True, vmem_limit_bytes=60 * 2**20
            ),
            name="attention",
        )(
            tokens, norm_gain.reshape(1, depth), gqw, gkw, gvw,
            gq_gain.reshape(1, HEAD), gk_gain.reshape(1, HEAD), lqw, lkw, lvw,
            sink, gow, low, jnp.asarray(row_tab), jnp.asarray(col_tab),
        )

    in_specs = (
        P("sp", None),
        P(),
        P(None, "tp"),
        P(None, "tp"),
        P(None, "tp"),
        P(),
        P(),
        P(None, "tp"),
        P(None, "tp"),
        P(None, "tp"),
        P("tp"),
        P("tp", None),
        P("tp", None),
    )
    out_specs = P(("sp", "tp"), None)
    return jax.shard_map(shards, mesh=mesh, in_specs=in_specs, out_specs=out_specs, check_vma=False)
```
